32 devices in a mesh: grp: 2 (over x), ep: 8 (over z, y), tp: 2 (over core).
Axes of the slice: x: 2, y: 2, z: 4, core: 2. Of those that a mesh axis runs over, the one named last changes fastest.
Arguments:
- tokens: bfloat16 [8192, 2048], P(('grp', 'ep', 'tp')), parts along dimension 0, may hold values from -6 to 6
- norm_gain: float32 [2048], replicated, may hold values from 0.1 to 1.9
- expert_ids: int32 [8192, 2], P(('grp', 'ep', 'tp')), parts along dimension 0, may hold values from 0 to 7, all different within a row; in each aligned block of 256 rows (0 to 255, 256 to 511, ...) at most 96 rows name the same one
- route_weights: float32 [8192, 2], P(('grp', 'ep', 'tp')), parts along dimension 0, may hold values from 0.05 to 1
- w_gate: bfloat16 [8, 2048, 1024], P('ep', None, 'tp'), may hold values from -0.125 to 0.125
- w_up: bfloat16 [8, 2048, 1024], P('ep', None, 'tp'), may hold values from -0.125 to 0.125
- w_down: bfloat16 [8, 1024, 2048], P('ep', 'tp'), may hold values from -0.1875 to 0.1875
Outputs:
- mixed: bfloat16 [8192, 2048], P(('grp', 'ep', 'tp')), parts along dimension 0
The draws below stay inside these ranges and needn't reach their ends.
There are 2 independent parts, one for each index of `grp`. The reference program is written for one: setup_inputs(seed, part) draws one part's arguments, and reference() takes and returns one part's arrays. A program takes and returns all parts, laid end to end along the dimension named above; an argument that names none is the same for every part. Nothing has to cross between parts.
Inputs may be any that keep to these rules, and one draw needn't show every extreme that they name: `expert_ids`: each row names 2 different experts. Among the rows of one device no expert is named more than 96 times, and in every draw some expert is named exactly 96 times by the rows of some device.
All inputs are finite; a program needn't handle non-finite values.
Results may differ from the reference program's by a relative error of at most 0.0071.
Values may be sent and summed in bfloat16 or wider, within the bound.
A program may use at most 128 MiB of HBM per device.

```python
import math
import jax
import jax.numpy as jnp
import numpy as np
from jax import lax

D = 2048
DE = 1024
TOP_K = 2
TOK_DEV = 256
EXPERTS = 8
TOKENS = 4096
CAP = 96


def block_scale(own_key, shape, pieces, low, top_value):
    def one(axis_at, blocks):
        heights = jax.random.uniform(jax.random.fold_in(jax.random.fold_in(own_key, 6), axis_at), (blocks,), jnp.float32, low / len(pieces), top_value / len(pieces))
        return jnp.repeat(jnp.exp(heights), shape[axis_at] // blocks).reshape((-1,) + (1,) * (len(shape) - axis_at - 1))

    factor_of = one(*pieces[0])
    for cut in pieces[1:]:
        factor_of = factor_of * one(*cut)
    return factor_of


def assign_block(own_key, own, number, rows, amount, top, most, skew):
    ranking = jax.random.permutation(own_key, amount)
    crowded, usual = shares(amount, rows * top, most, skew, True), shares(amount, rows * top, most, skew, False)
    places = jnp.arange(amount)

    def named(lengths, rotation):
        used = int((lengths > 0).sum())
        fixed = max(1, used // 4)
        moved = fixed + (places - fixed + rotation * (used - fixed)) % max(1, amount - fixed)
        return jnp.zeros((amount,), jnp.int32).at[ranking[jnp.where(places < fixed, places, moved)]].set(jnp.asarray(lengths, jnp.int32))

    lengths = jnp.where(number % 4 == 0, named(crowded, number // 4), named(usual, number - number // 4 - 1))
    mixed = jax.random.permutation(jax.random.fold_in(own, 3), amount)
    donor, taker = mixed[0:amount // 2 * 2:2], mixed[1:amount // 2 * 2:2]
    margin = jnp.minimum(lengths[donor] - 1, most - lengths[taker]) // 2
    margin = jnp.where((donor == ranking[0]) | (taker == ranking[0]) | (lengths[taker] == 0), 0, jnp.maximum(margin, 0))
    moved = jax.random.randint(jax.random.fold_in(own, 4), (amount // 2,), 0, 1 << 20) % (margin + 1)
    lengths = lengths.at[donor].add(-moved).at[taker].add(moved)
    items = jnp.searchsorted(jnp.cumsum(lengths), jnp.arange(rows * top), side="right").astype(jnp.int32)
    table = items.reshape(top, rows).T
    table = table[jax.random.permutation(jax.random.fold_in(own, 1), rows)]
    rotation = jax.random.randint(jax.random.fold_in(own, 2), (rows, 1), 0, top)
    return jnp.take_along_axis(table, (jnp.arange(top)[None, :] + rotation) % top, axis=1)


def shares(count, total, reach, lean, full):
    portions = [(1 << 20) // math.isqrt(grade ** lean) + 1 for grade in range(1, count + 1)]
    largest = reach if full else min(reach, max(-(-total // count), total * portions[0] // sum(portions)))
    least = 1 if total - largest >= count - 1 else 0
    given, surplus = [largest] + [least] * (count - 1), total - largest - least * (count - 1)
    while surplus > 0:
        candidates = [i for i in range(1, count) if given[i] < largest] or [i for i in range(1, count) if given[i] < reach]
        whole, budget = sum([portions[i] for i in candidates]), surplus
        for i in candidates:
            addition = min(reach - given[i], max(1, budget * portions[i] // whole), surplus)
            given[i] = given[i] + addition
            surplus = surplus - addition
    return np.array(given)


def centred(stream_key, shape, deviation, reach, shards=(), kind=jnp.bfloat16):
    entries = jax.random.normal(stream_key, shape, jnp.float32) * deviation
    if len(shards) > 0:
        entries = block_scale(stream_key, shape, shards, -0.22, 0.18) * entries
    return jnp.clip(entries, min=-reach, max=reach).astype(kind)


def setup_inputs(seed: int = 0, part: int = 0) -> dict:
    arg_keys = jax.random.split(jax.random.key(seed), 8)
    part_splits = jax.random.split(jax.random.fold_in(arg_keys[7], part), 8)
    tokens = centred(part_splits[0], (TOKENS, D), 1.0, 6.0, ((0, 16),))
    norm_gain = jnp.clip(1.0 + 0.18 * jax.random.normal(arg_keys[1], (D,), jnp.float32), 0.1, 1.9)
    expert_ids_keys = jax.random.split(jax.random.fold_in(part_splits[2], 1), TOKENS // TOK_DEV)
    expert_ids_turns = jax.random.permutation(jax.random.fold_in(part_splits[2], 3), TOKENS // TOK_DEV)
    expert_ids = jax.vmap(lambda own, number: assign_block(jax.random.fold_in(part_splits[2], 2), own, number, TOK_DEV, EXPERTS, TOP_K, CAP, 2))(expert_ids_keys, expert_ids_turns).reshape((TOKENS, TOP_K))
    route_weights = jnp.clip(jnp.exp(math.log(1.0) - 2.9957323 * jax.random.uniform(part_splits[3], (TOKENS, TOP_K), jnp.float32) ** block_scale(part_splits[3], (TOKENS, TOP_K), ((0, 16),), -0.2, 0.2)), 0.05, 1.0)
    w_gate = centred(arg_keys[4], (EXPERTS, D, DE), D ** -0.5, 0.125, ((0, 8), (2, 2)))
    w_up = centred(arg_keys[5], (EXPERTS, D, DE), D ** -0.5, 0.125, ((0, 8), (2, 2)))
    w_down = centred(arg_keys[6], (EXPERTS, DE, D), DE ** -0.5, 0.1875, ((0, 8), (1, 2)))
    return dict(tokens=tokens, norm_gain=norm_gain, expert_ids=expert_ids, route_weights=route_weights, w_gate=w_gate, w_up=w_up, w_down=w_down)


def reference(tokens, norm_gain, expert_ids, route_weights, w_gate, w_up, w_down):
    values = tokens.astype(jnp.float32)
    scale = lax.rsqrt(lax.optimization_barrier(jnp.mean(values * values, axis=-1, keepdims=True)) + 1e-06)
    normed = (values * scale * norm_gain).astype(jnp.bfloat16)
    flat_ids = expert_ids.reshape(-1)
    flat_weights = route_weights.reshape(-1)
    total_rows = TOKENS // TOK_DEV * CAP

    def per_expert(carry, expert):
        chosen = flat_ids == expert
        count = jnp.sum(chosen.astype(jnp.int32))
        picks = jnp.nonzero(chosen, size=total_rows, fill_value=0)[0].astype(jnp.int32)
        live = jnp.arange(total_rows, dtype=jnp.int32) < count
        token_rows = picks // TOP_K
        rows = normed[token_rows]
        gate = jnp.dot(rows, w_gate[expert], preferred_element_type=jnp.float32)
        upper = jnp.dot(rows, w_up[expert], preferred_element_type=jnp.float32)
        hidden = (jax.nn.silu(gate) * upper).astype(jnp.bfloat16)
        result = jnp.dot(hidden, w_down[expert], preferred_element_type=jnp.float32).astype(jnp.bfloat16)
        result = lax.optimization_barrier(result).astype(jnp.float32)
        weight = jnp.where(live, flat_weights[picks], jnp.float32(0.0))
        carry = carry.at[token_rows].add(weight[:, None] * result)
        return (carry, None)
    start = jnp.zeros((TOKENS, D), jnp.float32)
    total, _ = lax.scan(per_expert, start, jnp.arange(EXPERTS, dtype=jnp.int32))
    return total.astype(jnp.bfloat16)
```

```python
import functools

import jax
import jax.numpy as jnp
from jax import lax
from jax.experimental import pallas as pl
from jax.experimental.pallas import tpu as pltpu
from jax.sharding import PartitionSpec as P

MESH = pl.DeviceIdType.MESH
F32 = jnp.float32
BF16 = jnp.bfloat16


def plain_device(tokens, norm_gain, expert_ids, route_weights, w_gate, w_up, w_down):
    tok_rows = tokens.shape[0]
    top_count = expert_ids.shape[1]
    width = tokens.shape[1]
    local_experts = w_gate.shape[0]
    ep_size = lax.axis_size("ep")
    experts = local_experts * ep_size
    slots = 3 * tok_rows * top_count // (2 * experts)
    values = tokens.astype(jnp.float32)
    scale = lax.rsqrt(jnp.mean(values * values, axis=-1, keepdims=True) + 1e-06)
    normed = (values * scale * norm_gain).astype(jnp.bfloat16)
    flat_ids = expert_ids.reshape(-1)
    onehot = (flat_ids[:, None] == jnp.arange(experts, dtype=jnp.int32)[None, :]).astype(jnp.int32)
    before = jnp.cumsum(onehot, axis=0) - onehot
    slot_of = jnp.sum(before * onehot, axis=1)
    target = flat_ids * slots + slot_of
    owner = jnp.arange(tok_rows * top_count, dtype=jnp.int32) // top_count + 1
    source = jnp.zeros((experts * slots,), jnp.int32).at[target].set(owner)
    filled = source > 0
    picked = jnp.take(normed, jnp.maximum(source - 1, 0), axis=0)
    outgoing = jnp.where(filled[:, None], picked, jnp.zeros_like(picked))
    outgoing = outgoing.reshape(ep_size, local_experts, slots, width)
    gate_full, up_full = (
        lax.all_gather(w_gate, "tp", axis=2, tiled=True),
        lax.all_gather(w_up, "tp", axis=2, tiled=True),
    )
    down_full = lax.all_gather(w_down, "tp", axis=1, tiled=True)
    arrived = lax.all_to_all(outgoing, "ep", split_axis=0, concat_axis=0, tiled=True)
    senders, _, part_slots, _ = arrived.shape
    rows = jnp.transpose(arrived, (1, 0, 2, 3)).reshape(local_experts, senders * part_slots, width)
    gate = jnp.einsum("erd,edf->erf", rows, gate_full, preferred_element_type=jnp.float32)
    upper = jnp.einsum("erd,edf->erf", rows, up_full, preferred_element_type=jnp.float32)
    hidden = (jax.nn.silu(gate) * upper).astype(jnp.bfloat16)
    result = jnp.einsum(
        "erf,efd->erd", hidden, down_full, preferred_element_type=jnp.float32
    ).astype(jnp.bfloat16)
    result = result.reshape(local_experts, senders, part_slots, width)
    result = jnp.transpose(result, (1, 0, 2, 3))
    results = lax.all_to_all(result, "ep", split_axis=0, concat_axis=0, tiled=True)
    results = results.reshape(experts * slots, width)
    gathered = jnp.take(results, target, axis=0).reshape(tok_rows, top_count, width)
    mixed = jnp.sum(route_weights[:, :, None] * gathered.astype(jnp.float32), axis=1)
    return mixed.astype(jnp.bfloat16)


def flip(me, d, ep):
    out, bit = 0, 1
    while bit < ep:
        out = out + bit * ((me // bit + d // bit) % 2)
        bit *= 2
    return out


def kernel(
    ep, slots, tok, gain, ids, rw, wg, wu, wd, o_ref,
    gbuf, ubuf, dbuf, normed, out, recv, hid, res, back, acc,
    w_sem, ws_sem, wr_sem, s1, r1, s2, r2,
):
    me = lax.axis_index("ep")
    tp = lax.axis_index("tp")
    rows, width = tok.shape
    half = wg.shape[2]
    tile = min(512, width)
    mine = pl.ds(pl.multiple_of(tp * half, 128), half)

    barrier = pltpu.get_barrier_semaphore()
    for d in range(1, ep):
        pl.semaphore_signal(barrier, inc=1, device_id={"ep": flip(me, d, ep)}, device_id_type=MESH)
    pl.semaphore_signal(barrier, inc=1, device_id={"tp": 1 - tp}, device_id_type=MESH)

    weights = [
        (wg.at[0], gbuf.at[tp]),
        (wu.at[0], ubuf.at[tp]),
        (wd.at[0], dbuf.at[mine]),
    ]
    local = [pltpu.make_async_copy(a, b, w_sem.at[i]) for i, (a, b) in enumerate(weights)]
    for c in local:
        c.start()

    @pl.loop(0, rows // 16)
    def _(i):
        at = pl.ds(pl.multiple_of(i * 16, 16), 16)
        v = tok[at, :].astype(F32)
        scale = lax.rsqrt(jnp.mean(v * v, axis=-1, keepdims=True) + 1e-06)
        normed[at, :] = (v * scale * gain[...]).astype(BF16)

    lane = lax.broadcasted_iota(jnp.int32, (rows, 128), 1)
    rel = ids[...] ^ me
    hits = [rel[:, k:k + 1] == lane for k in range(ids.shape[1])]
    member = jnp.zeros((rows, 128), F32)
    share = jnp.zeros((rows, 128), F32)
    for k, hit in enumerate(hits):
        member = member + jnp.where(hit, 1.0, 0.0)
        share = share + jnp.where(hit, rw[:, k:k + 1], 0.0)
    later = lax.broadcasted_iota(jnp.int32, (rows, rows), 0)
    earlier = lax.broadcasted_iota(jnp.int32, (rows, rows), 1)
    below = jnp.where(earlier < later, 1.0, 0.0).astype(BF16)
    rank = jnp.dot(below, member.astype(BF16), preferred_element_type=F32)
    key = member * (rank + 1.0) - 1.0
    key_t = key.T
    key = key.astype(jnp.int32)
    key_t = key_t.astype(jnp.int32)

    def pick(d, dst, base):
        spot = lax.broadcasted_iota(jnp.int32, (slots, rows), 0)
        sel = jnp.where(spot == key_t[d:d + 1, :], 1.0, 0.0).astype(BF16)

        @pl.loop(0, width // tile)
        def _(j):
            c = pl.ds(pl.multiple_of(j * tile, tile), tile)
            dst[pl.ds(base, slots), c] = jnp.dot(
                sel, normed[:, c], preferred_element_type=F32
            ).astype(BF16)

    def send_rows(d):
        at = pl.ds(pl.multiple_of(d * slots, 16), slots)
        return pltpu.make_async_remote_copy(
            src_ref=out.at[at], dst_ref=recv.at[at], send_sem=s1.at[d], recv_sem=r1.at[d],
            device_id={"ep": flip(me, d, ep)}, device_id_type=MESH,
        )

    def send_back(d):
        at = pl.ds(pl.multiple_of(d * slots, 16), slots)
        return pltpu.make_async_remote_copy(
            src_ref=res.at[at], dst_ref=back.at[at], send_sem=s2.at[d], recv_sem=r2.at[d],
            device_id={"ep": flip(me, d, ep)}, device_id_type=MESH,
        )

    pl.semaphore_wait(barrier, ep)

    order = range(1, ep)
    for d in order:
        pick(d, out, d * slots)
        send_rows(d).start()
    passed = [
        pltpu.make_async_remote_copy(
            src_ref=a, dst_ref=b, send_sem=ws_sem.at[i], recv_sem=wr_sem.at[i],
            device_id={"tp": 1 - tp}, device_id_type=MESH,
        )
        for i, (a, b) in enumerate(weights)
    ]
    for c in passed:
        c.start()
    pick(0, recv, 0)
    for c in local:
        c.wait()
    for c in passed:
        c.wait_recv()

    def work(p):
        at = pl.ds(pl.multiple_of(p * 2 * slots, 16), 2 * slots)
        nt = 256
        for h in range(2):
            for n in range(half // nt):
                c = slice(n * nt, (n + 1) * nt)
                x = recv[at, :]
                g = jnp.dot(x, gbuf[h, :, c], preferred_element_type=F32)
                u = jnp.dot(x, ubuf[h, :, c], preferred_element_type=F32)
                v = g / (1.0 + jnp.exp(-g)) * u
                hid[:, h * half + n * nt:h * half + (n + 1) * nt] = v.astype(BF16)

        @pl.loop(0, width // tile)
        def _(j):
            c = pl.ds(pl.multiple_of(j * tile, tile), tile)
            res[at, c] = jnp.dot(hid[...], dbuf[:, c], preferred_element_type=F32).astype(BF16)

    send_rows(1).wait_recv()
    work(0)
    send_back(1).start()

    @pl.loop(1, ep // 2)
    def _(p):
        send_rows(2 * p).wait_recv()
        send_rows(2 * p + 1).wait_recv()
        work(p)
        send_back(2 * p).start()
        send_back(2 * p + 1).start()

    def mix(d, src):
        slot = lax.broadcasted_iota(jnp.int32, (rows, slots), 1)
        sel = jnp.where(slot == key[:, d:d + 1], 1.0, 0.0).astype(BF16)
        part = share[:, d:d + 1]

        @pl.loop(0, width // tile)
        def _(j):
            c = pl.ds(pl.multiple_of(j * tile, tile), tile)
            y = part * jnp.dot(
                sel, src[pl.ds(d * slots, slots), c], preferred_element_type=F32
            )
            if d == 0:
                acc[:, c] = y
            elif d < ep - 1:
                acc[:, c] = acc[:, c] + y
            else:
                o_ref[:, c] = (acc[:, c] + y).astype(BF16)

    mix(0, res)
    for d in range(1, ep):
        send_back(d).wait_recv()
        mix(d, back)
    for d in range(1, ep):
        send_rows(d).wait_send()
        send_back(d).wait_send()
    for c in passed:
        c.wait_send()


def fused_device(tokens, norm_gain, expert_ids, route_weights, w_gate, w_up, w_down):
    rows, width = tokens.shape
    ep = lax.axis_size("ep")
    tps = lax.axis_size("tp")
    slots = 3 * rows * expert_ids.shape[1] // (2 * ep)
    half = w_gate.shape[2]
    vm = pl.BlockSpec(memory_space=pltpu.VMEM)
    anywhere = pl.BlockSpec(memory_space=pl.ANY)
    dma = pltpu.SemaphoreType.DMA
    return pl.pallas_call(
        functools.partial(kernel, ep, slots),
        out_shape=jax.ShapeDtypeStruct((rows, width), BF16),
        in_specs=[vm, vm, vm, vm, anywhere, anywhere, anywhere],
        out_specs=vm,
        scratch_shapes=[
            pltpu.VMEM((tps, width, half), BF16),
            pltpu.VMEM((tps, width, half), BF16),
            pltpu.VMEM((tps * half, width), BF16),
            pltpu.VMEM((rows, width), BF16),
            pltpu.VMEM((ep * slots, width), BF16),
            pltpu.VMEM((ep * slots, width), BF16),
            pltpu.VMEM((2 * slots, tps * half), BF16),
            pltpu.VMEM((ep * slots, width), BF16),
            pltpu.VMEM((ep * slots, width), BF16),
            pltpu.VMEM((rows, width), F32),
            dma((3,)), dma((3,)), dma((3,)),
            dma((ep,)), dma((ep,)), dma((ep,)), dma((ep,)),
        ],
        compiler_params=pltpu.CompilerParams(
            collective_id=0, has_side_effects=True, vmem_limit_bytes=56 * 1024 * 1024
        ),
    )(tokens, norm_gain.reshape(1, -1), expert_ids, route_weights, w_gate, w_up, w_down)


def per_device(tokens, norm_gain, expert_ids, route_weights, w_gate, w_up, w_down):
    rows, width = tokens.shape
    ep = lax.axis_size("ep")
    slots = 3 * rows * expert_ids.shape[1] // (2 * ep)
    fits = (
        w_gate.shape[0] == 1
        and lax.axis_size("tp") == 2
        and ep & (ep - 1) == 0
        and ep <= 128
        and slots % 16 == 0
        and rows % 128 == 0
        and width % 512 == 0
        and w_gate.shape[2] % 256 == 0
    )
    body = fused_device if fits else plain_device
    return body(tokens, norm_gain, expert_ids, route_weights, w_gate, w_up, w_down)


def solution(mesh):
    in_specs = (
        P(("grp", "ep", "tp"), None),
        P(),
        P(("grp", "ep", "tp"), None),
        P(("grp", "ep", "tp"), None),
        P("ep", None, "tp"),
        P("ep", None, "tp"),
        P("ep", "tp", None),
    )
    out_specs = P(("grp", "ep", "tp"), None)
    return jax.shard_map(
        per_device, mesh=mesh, in_specs=in_specs, out_specs=out_specs, check_vma=False
    )
```

```python
import functools

import jax
import jax.numpy as jnp
from jax import lax
from jax.experimental import pallas as pl
from jax.experimental.pallas import tpu as pltpu
from jax.sharding import PartitionSpec as P

MESH = pl.DeviceIdType.MESH
F32 = jnp.float32
BF16 = jnp.bfloat16


def plain_device(tokens, norm_gain, expert_ids, route_weights, w_gate, w_up, w_down):
    tok_rows = tokens.shape[0]
    top_count = expert_ids.shape[1]
    width = tokens.shape[1]
    local_experts = w_gate.shape[0]
    ep_size = lax.axis_size("ep")
    experts = local_experts * ep_size
    slots = 3 * tok_rows * top_count // (2 * experts)
    values = tokens.astype(jnp.float32)
    scale = lax.rsqrt(jnp.mean(values * values, axis=-1, keepdims=True) + 1e-06)
    normed = (values * scale * norm_gain).astype(jnp.bfloat16)
    flat_ids = expert_ids.reshape(-1)
    onehot = (flat_ids[:, None] == jnp.arange(experts, dtype=jnp.int32)[None, :]).astype(jnp.int32)
    before = jnp.cumsum(onehot, axis=0) - onehot
    slot_of = jnp.sum(before * onehot, axis=1)
    target = flat_ids * slots + slot_of
    owner = jnp.arange(tok_rows * top_count, dtype=jnp.int32) // top_count + 1
    source = jnp.zeros((experts * slots,), jnp.int32).at[target].set(owner)
    filled = source > 0
    picked = jnp.take(normed, jnp.maximum(source - 1, 0), axis=0)
    outgoing = jnp.where(filled[:, None], picked, jnp.zeros_like(picked))
    outgoing = outgoing.reshape(ep_size, local_experts, slots, width)
    gate_full, up_full = (
        lax.all_gather(w_gate, "tp", axis=2, tiled=True),
        lax.all_gather(w_up, "tp", axis=2, tiled=True),
    )
    down_full = lax.all_gather(w_down, "tp", axis=1, tiled=True)
    arrived = lax.all_to_all(outgoing, "ep", split_axis=0, concat_axis=0, tiled=True)
    senders, _, part_slots, _ = arrived.shape
    rows = jnp.transpose(arrived, (1, 0, 2, 3)).reshape(local_experts, senders * part_slots, width)
    gate = jnp.einsum("erd,edf->erf", rows, gate_full, preferred_element_type=jnp.float32)
    upper = jnp.einsum("erd,edf->erf", rows, up_full, preferred_element_type=jnp.float32)
    hidden = (jax.nn.silu(gate) * upper).astype(jnp.bfloat16)
    result = jnp.einsum(
        "erf,efd->erd", hidden, down_full, preferred_element_type=jnp.float32
    ).astype(jnp.bfloat16)
    result = result.reshape(local_experts, senders, part_slots, width)
    result = jnp.transpose(result, (1, 0, 2, 3))
    results = lax.all_to_all(result, "ep", split_axis=0, concat_axis=0, tiled=True)
    results = results.reshape(experts * slots, width)
    gathered = jnp.take(results, target, axis=0).reshape(tok_rows, top_count, width)
    mixed = jnp.sum(route_weights[:, :, None] * gathered.astype(jnp.float32), axis=1)
    return mixed.astype(jnp.bfloat16)


def flip(me, d, ep):
    out, bit = 0, 1
    while bit < ep:
        out = out + bit * ((me // bit + d // bit) % 2)
        bit *= 2
    return out


def kernel(
    ep, slots, tok, gain, ids, rw, wg, wu, wd, o_ref,
    gbuf, ubuf, dbuf, normed, out, recv, hid, res, back, acc,
    meta, meta_in, joined, joined_in,
    w_sem, ws_sem, wr_sem, s1, r1, s2, r2, s3, r3,
):
    me = lax.axis_index("ep")
    tp = lax.axis_index("tp")
    far = ep // 2
    inner = (me // (far // 2) + me // far) % 2
    rows, width = tok.shape
    half = wg.shape[2]
    tile = min(512, width)
    mine = pl.ds(pl.multiple_of(tp * half, 128), half)

    barrier = pltpu.get_barrier_semaphore()
    for d in range(1, ep):
        pl.semaphore_signal(barrier, inc=1, device_id={"ep": flip(me, d, ep)}, device_id_type=MESH)
    pl.semaphore_signal(barrier, inc=1, device_id={"tp": 1 - tp}, device_id_type=MESH)

    weights = [
        (wg.at[0], gbuf.at[tp]),
        (wu.at[0], ubuf.at[tp]),
        (wd.at[0], dbuf.at[mine]),
    ]
    local = [pltpu.make_async_copy(a, b, w_sem.at[i]) for i, (a, b) in enumerate(weights)]
    for c in local:
        c.start()

    @pl.loop(0, rows // 16)
    def _(i):
        at = pl.ds(pl.multiple_of(i * 16, 16), 16)
        v = tok[at, :].astype(F32)
        scale = lax.rsqrt(jnp.mean(v * v, axis=-1, keepdims=True) + 1e-06)
        normed[at, :] = (v * scale * gain[...]).astype(BF16)

    lane = lax.broadcasted_iota(jnp.int32, (rows, 128), 1)
    rel = ids[...] ^ me
    hits = [rel[:, k:k + 1] == lane for k in range(ids.shape[1])]
    member = jnp.zeros((rows, 128), F32)
    share = jnp.zeros((rows, 128), F32)
    for k, hit in enumerate(hits):
        member = member + jnp.where(hit, 1.0, 0.0)
        share = share + jnp.where(hit, rw[:, k:k + 1], 0.0)
    later = lax.broadcasted_iota(jnp.int32, (rows, rows), 0)
    earlier = lax.broadcasted_iota(jnp.int32, (rows, rows), 1)
    below = jnp.where(earlier < later, 1.0, 0.0).astype(BF16)
    rank = jnp.dot(below, member.astype(BF16), preferred_element_type=F32)
    key = member * (rank + 1.0) - 1.0
    key_t = key.T
    meta[0:ep, :] = key_t[0:ep, :]
    meta[ep:2 * ep, :] = share.T[0:ep, :]
    key = key.astype(jnp.int32)
    key_t = key_t.astype(jnp.int32)

    def pick(d, dst, base):
        spot = lax.broadcasted_iota(jnp.int32, (slots, rows), 0)
        sel = jnp.where(spot == key_t[d:d + 1, :], 1.0, 0.0).astype(BF16)

        @pl.loop(0, width // tile)
        def _(j):
            c = pl.ds(pl.multiple_of(j * tile, tile), tile)
            dst[pl.ds(base, slots), c] = jnp.dot(
                sel, normed[:, c], preferred_element_type=F32
            ).astype(BF16)

    def send_rows(d):
        at = pl.ds(pl.multiple_of(d * slots, 16), slots)
        return pltpu.make_async_remote_copy(
            src_ref=out.at[at], dst_ref=recv.at[at], send_sem=s1.at[d], recv_sem=r1.at[d],
            device_id={"ep": flip(me, d, ep)}, device_id_type=MESH,
        )

    def send_back(d, to):
        at = pl.ds(pl.multiple_of(d * slots, 16), slots)
        return pltpu.make_async_remote_copy(
            src_ref=res.at[at], dst_ref=back.at[at], send_sem=s2.at[d], recv_sem=r2.at[d],
            device_id={"ep": flip(me, to, ep)}, device_id_type=MESH,
        )

    def across(i, src, dst):
        return pltpu.make_async_remote_copy(
            src_ref=src, dst_ref=dst, send_sem=s3.at[i], recv_sem=r3.at[i],
            device_id={"ep": flip(me, far, ep)}, device_id_type=MESH,
        )

    pl.semaphore_wait(barrier, ep)

    told = across(0, meta, meta_in)
    told.start()
    distant = [d for p in reversed(range(far, ep, 2)) for d in (p, p + 1)]
    for d in distant:
        pick(d, out, d * slots)

        @pl.when(inner == 1)
        def _():
            send_rows(d).start()

    for d in range(1, far):
        pick(d, out, d * slots)
        send_rows(d).start()
    passed = [
        pltpu.make_async_remote_copy(
            src_ref=a, dst_ref=b, send_sem=ws_sem.at[i], recv_sem=wr_sem.at[i],
            device_id={"tp": 1 - tp}, device_id_type=MESH,
        )
        for i, (a, b) in enumerate(weights)
    ]
    for c in passed:
        c.start()
    pick(0, recv, 0)
    for c in local:
        c.wait()
    for c in passed:
        c.wait_recv()

    def work(p):
        at = pl.ds(pl.multiple_of(p * 2 * slots, 16), 2 * slots)
        nt = 256
        for h in range(2):
            for n in range(half // nt):
                c = slice(n * nt, (n + 1) * nt)
                x = recv[at, :]
                g = jnp.dot(x, gbuf[h, :, c], preferred_element_type=F32)
                u = jnp.dot(x, ubuf[h, :, c], preferred_element_type=F32)
                v = g / (1.0 + jnp.exp(-g)) * u
                hid[:, h * half + n * nt:h * half + (n + 1) * nt] = v.astype(BF16)

        @pl.loop(0, width // tile)
        def _(j):
            c = pl.ds(pl.multiple_of(j * tile, tile), tile)
            res[at, c] = jnp.dot(hid[...], dbuf[:, c], preferred_element_type=F32).astype(BF16)

    send_rows(1).wait_recv()
    work(0)
    send_back(1, 1).start()

    @pl.loop(1, far // 2)
    def _(p):
        send_rows(2 * p).wait_recv()
        send_rows(2 * p + 1).wait_recv()
        work(p)
        send_back(2 * p, 2 * p).start()
        send_back(2 * p + 1, 2 * p + 1).start()

    @pl.when(inner == 0)
    def _():
        for d in distant:
            send_rows(d).start()

    pairs = ep // 4

    @pl.loop(0, pairs)
    def _(i):
        q = (i + inner) % pairs
        d = far + 2 * q
        send_rows(d).wait_recv()
        send_rows(d + 1).wait_recv()
        work(far // 2 + q)

        @pl.when(q > 0)
        def _():
            send_back(d, 2 * q).start()

        send_back(d + 1, 2 * q + 1).start()

    def mix(d, src, slot_of, part_of, first, dst):
        slot = lax.broadcasted_iota(jnp.int32, (rows, slots), 1)
        sel = jnp.where(slot == slot_of[:, d:d + 1], 1.0, 0.0).astype(BF16)

        @pl.loop(0, width // tile)
        def _(j):
            c = pl.ds(pl.multiple_of(j * tile, tile), tile)
            y = part_of * jnp.dot(
                sel, src[pl.ds(d * slots, slots), c], preferred_element_type=F32
            )
            if not first:
                y = acc[:, c] + y
            if dst is None:
                acc[:, c] = y
            else:
                dst[:, c] = y.astype(BF16)

    told.wait_recv()
    blank = jnp.zeros((128 - 2 * ep, rows), F32)
    theirs = jnp.concatenate([meta_in[...], blank], axis=0).T
    slot_theirs = theirs.astype(jnp.int32)
    for d in range(far, ep):
        if d > far:
            send_back(d, d - far).wait_recv()
        mix(
            d, res if d == far else back, slot_theirs, theirs[:, ep + d:ep + d + 1],
            d == far, joined if d == ep - 1 else None,
        )
    home = across(1, joined, joined_in)
    home.start()

    for d in range(far):
        if d > 0:
            send_back(d, d).wait_recv()
        mix(d, res if d == 0 else back, key, share[:, d:d + 1], d == 0, None)
    home.wait_recv()

    @pl.loop(0, width // tile)
    def _(j):
        c = pl.ds(pl.multiple_of(j * tile, tile), tile)
        o_ref[:, c] = (acc[:, c] + joined_in[:, c].astype(F32)).astype(BF16)

    for d in range(1, ep):
        send_rows(d).wait_send()
        if d < far:
            send_back(d, d).wait_send()
        elif d > far:
            send_back(d, d - far).wait_send()
    told.wait_send()
    home.wait_send()
    for c in passed:
        c.wait_send()


def fused_device(tokens, norm_gain, expert_ids, route_weights, w_gate, w_up, w_down):
    rows, width = tokens.shape
    ep = lax.axis_size("ep")
    tps = lax.axis_size("tp")
    slots = 3 * rows * expert_ids.shape[1] // (2 * ep)
    half = w_gate.shape[2]
    vm = pl.BlockSpec(memory_space=pltpu.VMEM)
    anywhere = pl.BlockSpec(memory_space=pl.ANY)
    dma = pltpu.SemaphoreType.DMA
    return pl.pallas_call(
        functools.partial(kernel, ep, slots),
        out_shape=jax.ShapeDtypeStruct((rows, width), BF16),
        in_specs=[vm, vm, vm, vm, anywhere, anywhere, anywhere],
        out_specs=vm,
        scratch_shapes=[
            pltpu.VMEM((tps, width, half), BF16),
            pltpu.VMEM((tps, width, half), BF16),
            pltpu.VMEM((tps * half, width), BF16),
            pltpu.VMEM((rows, width), BF16),
            pltpu.VMEM((ep * slots, width), BF16),
            pltpu.VMEM((ep * slots, width), BF16),
            pltpu.VMEM((2 * slots, tps * half), BF16),
            pltpu.VMEM((ep * slots, width), BF16),
            pltpu.VMEM((ep * slots, width), BF16),
            pltpu.VMEM((rows, width), F32),
            pltpu.VMEM((2 * ep, rows), F32),
            pltpu.VMEM((2 * ep, rows), F32),
            pltpu.VMEM((rows, width), BF16),
            pltpu.VMEM((rows, width), BF16),
            dma((3,)), dma((3,)), dma((3,)),
            dma((ep,)), dma((ep,)), dma((ep,)), dma((ep,)), dma((2,)), dma((2,)),
        ],
        compiler_params=pltpu.CompilerParams(
            collective_id=0, has_side_effects=True, vmem_limit_bytes=56 * 1024 * 1024
        ),
    )(tokens, norm_gain.reshape(1, -1), expert_ids, route_weights, w_gate, w_up, w_down)


def per_device(tokens, norm_gain, expert_ids, route_weights, w_gate, w_up, w_down):
    rows, width = tokens.shape
    ep = lax.axis_size("ep")
    slots = 3 * rows * expert_ids.shape[1] // (2 * ep)
    fits = (
        w_gate.shape[0] == 1
        and lax.axis_size("tp") == 2
        and ep & (ep - 1) == 0
        and 8 <= ep <= 32
        and slots % 16 == 0
        and rows % 128 == 0
        and width % 512 == 0
        and w_gate.shape[2] % 256 == 0
    )
    body = fused_device if fits else plain_device
    return body(tokens, norm_gain, expert_ids, route_weights, w_gate, w_up, w_down)


def solution(mesh):
    in_specs = (
        P(("grp", "ep", "tp"), None),
        P(),
        P(("grp", "ep", "tp"), None),
        P(("grp", "ep", "tp"), None),
        P("ep", None, "tp"),
        P("ep", None, "tp"),
        P("ep", "tp", None),
    )
    out_specs = P(("grp", "ep", "tp"), None)
    return jax.shard_map(
        per_device, mesh=mesh, in_specs=in_specs, out_specs=out_specs, check_vma=False
    )
```

```python
import functools

import jax
import jax.numpy as jnp
from jax import lax
from jax.experimental import pallas as pl
from jax.experimental.pallas import tpu as pltpu
from jax.sharding import PartitionSpec as P

MESH = pl.DeviceIdType.MESH
F32 = jnp.float32
BF16 = jnp.bfloat16


def plain_device(tokens, norm_gain, expert_ids, route_weights, w_gate, w_up, w_down):
    tok_rows = tokens.shape[0]
    top_count = expert_ids.shape[1]
    width = tokens.shape[1]
    local_experts = w_gate.shape[0]
    ep_size = lax.axis_size("ep")
    experts = local_experts * ep_size
    slots = 3 * tok_rows * top_count // (2 * experts)
    values = tokens.astype(jnp.float32)
    scale = lax.rsqrt(jnp.mean(values * values, axis=-1, keepdims=True) + 1e-06)
    normed = (values * scale * norm_gain).astype(jnp.bfloat16)
    flat_ids = expert_ids.reshape(-1)
    onehot = (flat_ids[:, None] == jnp.arange(experts, dtype=jnp.int32)[None, :]).astype(jnp.int32)
    before = jnp.cumsum(onehot, axis=0) - onehot
    slot_of = jnp.sum(before * onehot, axis=1)
    target = flat_ids * slots + slot_of
    owner = jnp.arange(tok_rows * top_count, dtype=jnp.int32) // top_count + 1
    source = jnp.zeros((experts * slots,), jnp.int32).at[target].set(owner)
    filled = source > 0
    picked = jnp.take(normed, jnp.maximum(source - 1, 0), axis=0)
    outgoing = jnp.where(filled[:, None], picked, jnp.zeros_like(picked))
    outgoing = outgoing.reshape(ep_size, local_experts, slots, width)
    gate_full, up_full = (
        lax.all_gather(w_gate, "tp", axis=2, tiled=True),
        lax.all_gather(w_up, "tp", axis=2, tiled=True),
    )
    down_full = lax.all_gather(w_down, "tp", axis=1, tiled=True)
    arrived = lax.all_to_all(outgoing, "ep", split_axis=0, concat_axis=0, tiled=True)
    senders, _, part_slots, _ = arrived.shape
    rows = jnp.transpose(arrived, (1, 0, 2, 3)).reshape(local_experts, senders * part_slots, width)
    gate = jnp.einsum("erd,edf->erf", rows, gate_full, preferred_element_type=jnp.float32)
    upper = jnp.einsum("erd,edf->erf", rows, up_full, preferred_element_type=jnp.float32)
    hidden = (jax.nn.silu(gate) * upper).astype(jnp.bfloat16)
    result = jnp.einsum(
        "erf,efd->erd", hidden, down_full, preferred_element_type=jnp.float32
    ).astype(jnp.bfloat16)
    result = result.reshape(local_experts, senders, part_slots, width)
    result = jnp.transpose(result, (1, 0, 2, 3))
    results = lax.all_to_all(result, "ep", split_axis=0, concat_axis=0, tiled=True)
    results = results.reshape(experts * slots, width)
    gathered = jnp.take(results, target, axis=0).reshape(tok_rows, top_count, width)
    mixed = jnp.sum(route_weights[:, :, None] * gathered.astype(jnp.float32), axis=1)
    return mixed.astype(jnp.bfloat16)


def flip(me, d, ep):
    out, bit = 0, 1
    while bit < ep:
        out = out + bit * ((me // bit + d // bit) % 2)
        bit *= 2
    return out


def kernel(
    ep, slots, tok, gain, ids, rw, wg, wu, wd, o_ref,
    gbuf, ubuf, dbuf, normed, out, recv, hid, res, back, acc,
    meta, meta_in, joined, joined_in,
    w_sem, ws_sem, wr_sem, s1, r1, s2, r2, s3, r3,
):
    me = lax.axis_index("ep")
    tp = lax.axis_index("tp")
    far = ep // 2
    inner = (me // (far // 2) + me // far) % 2
    rows, width = tok.shape
    half = wg.shape[2]
    tile = min(512, width)
    mine = pl.ds(pl.multiple_of(tp * half, 128), half)

    barrier = pltpu.get_barrier_semaphore()
    for d in range(1, ep):
        pl.semaphore_signal(barrier, inc=1, device_id={"ep": flip(me, d, ep)}, device_id_type=MESH)
    pl.semaphore_signal(barrier, inc=1, device_id={"tp": 1 - tp}, device_id_type=MESH)

    weights = [
        (wg.at[0], gbuf.at[tp]),
        (wu.at[0], ubuf.at[tp]),
        (wd.at[0], dbuf.at[mine]),
    ]
    local = [pltpu.make_async_copy(a, b, w_sem.at[i]) for i, (a, b) in enumerate(weights)]
    for c in local:
        c.start()

    @pl.loop(0, rows // 16)
    def _(i):
        at = pl.ds(pl.multiple_of(i * 16, 16), 16)
        v = tok[at, :].astype(F32)
        scale = lax.rsqrt(jnp.mean(v * v, axis=-1, keepdims=True) + 1e-06)
        normed[at, :] = (v * scale * gain[...]).astype(BF16)

    lane = lax.broadcasted_iota(jnp.int32, (rows, 128), 1)
    rel = ids[...] ^ me
    hits = [rel[:, k:k + 1] == lane for k in range(ids.shape[1])]
    member = jnp.zeros((rows, 128), F32)
    share = jnp.zeros((rows, 128), F32)
    for k, hit in enumerate(hits):
        member = member + jnp.where(hit, 1.0, 0.0)
        share = share + jnp.where(hit, rw[:, k:k + 1], 0.0)
    later = lax.broadcasted_iota(jnp.int32, (rows, rows), 0)
    earlier = lax.broadcasted_iota(jnp.int32, (rows, rows), 1)
    below = jnp.where(earlier < later, 1.0, 0.0).astype(BF16)
    rank = jnp.dot(below, member.astype(BF16), preferred_element_type=F32)
    key = member * (rank + 1.0) - 1.0
    key_t = key.T
    meta[0:ep, :] = key_t[0:ep, :]
    meta[ep:2 * ep, :] = share.T[0:ep, :]
    key = key.astype(jnp.int32)
    key_t = key_t.astype(jnp.int32)

    def pick(d, dst, base):
        spot = lax.broadcasted_iota(jnp.int32, (slots, rows), 0)
        sel = jnp.where(spot == key_t[d:d + 1, :], 1.0, 0.0).astype(BF16)

        @pl.loop(0, width // tile)
        def _(j):
            c = pl.ds(pl.multiple_of(j * tile, tile), tile)
            dst[pl.ds(base, slots), c] = jnp.dot(
                sel, normed[:, c], preferred_element_type=F32
            ).astype(BF16)

    def send_rows(d):
        at = pl.ds(pl.multiple_of(d * slots, 16), slots)
        return pltpu.make_async_remote_copy(
            src_ref=out.at[at], dst_ref=recv.at[at], send_sem=s1.at[d], recv_sem=r1.at[d],
            device_id={"ep": flip(me, d, ep)}, device_id_type=MESH,
        )

    def send_back(d, to):
        at = pl.ds(pl.multiple_of(d * slots, 16), slots)
        return pltpu.make_async_remote_copy(
            src_ref=res.at[at], dst_ref=back.at[at], send_sem=s2.at[d], recv_sem=r2.at[d],
            device_id={"ep": flip(me, to, ep)}, device_id_type=MESH,
        )

    def across(i, src, dst):
        return pltpu.make_async_remote_copy(
            src_ref=src, dst_ref=dst, send_sem=s3.at[i], recv_sem=r3.at[i],
            device_id={"ep": flip(me, far, ep)}, device_id_type=MESH,
        )

    pl.semaphore_wait(barrier, ep)

    told = across(0, meta, meta_in)
    told.start()
    for d in range(1, far):
        pick(d, out, d * slots)
        send_rows(d).start()
    distant = [d for p in reversed(range(far, ep, 2)) for d in (p, p + 1)]
    for d in distant:
        pick(d, out, d * slots)

        @pl.when(inner == 1)
        def _():
            send_rows(d).start()
    passed = [
        pltpu.make_async_remote_copy(
            src_ref=a, dst_ref=b, send_sem=ws_sem.at[i], recv_sem=wr_sem.at[i],
            device_id={"tp": 1 - tp}, device_id_type=MESH,
        )
        for i, (a, b) in enumerate(weights)
    ]
    for c in passed:
        c.start()
    pick(0, recv, 0)
    for c in local:
        c.wait()
    for c in passed:
        c.wait_recv()

    def work(p):
        at = pl.ds(pl.multiple_of(p * 2 * slots, 16), 2 * slots)
        nt = 256
        for h in range(2):
            for n in range(half // nt):
                c = slice(n * nt, (n + 1) * nt)
                x = recv[at, :]
                g = jnp.dot(x, gbuf[h, :, c], preferred_element_type=F32)
                u = jnp.dot(x, ubuf[h, :, c], preferred_element_type=F32)
                v = g / (1.0 + jnp.exp(-g)) * u
                hid[:, h * half + n * nt:h * half + (n + 1) * nt] = v.astype(BF16)

        @pl.loop(0, width // tile)
        def _(j):
            c = pl.ds(pl.multiple_of(j * tile, tile), tile)
            res[at, c] = jnp.dot(hid[...], dbuf[:, c], preferred_element_type=F32).astype(BF16)

    send_rows(1).wait_recv()
    work(0)
    send_back(1, 1).start()

    @pl.when(inner == 0)
    def _():
        for d in distant:
            send_rows(d).start()

    @pl.loop(1, far // 2)
    def _(p):
        send_rows(2 * p).wait_recv()
        send_rows(2 * p + 1).wait_recv()
        work(p)
        send_back(2 * p, 2 * p).start()
        send_back(2 * p + 1, 2 * p + 1).start()

    pairs = ep // 4

    @pl.loop(0, pairs)
    def _(i):
        q = (i + inner) % pairs
        d = far + 2 * q
        send_rows(d).wait_recv()
        send_rows(d + 1).wait_recv()
        work(far // 2 + q)

        @pl.when(q > 0)
        def _():
            send_back(d, 2 * q).start()

        send_back(d + 1, 2 * q + 1).start()

    def mix(d, src, slot_of, part_of, first, dst):
        slot = lax.broadcasted_iota(jnp.int32, (rows, slots), 1)
        sel = jnp.where(slot == slot_of[:, d:d + 1], 1.0, 0.0).astype(BF16)

        @pl.loop(0, width // tile)
        def _(j):
            c = pl.ds(pl.multiple_of(j * tile, tile), tile)
            y = part_of * jnp.dot(
                sel, src[pl.ds(d * slots, slots), c], preferred_element_type=F32
            )
            if not first:
                y = acc[:, c] + y
            if dst is None:
                acc[:, c] = y
            else:
                dst[:, c] = y.astype(BF16)

    told.wait_recv()
    blank = jnp.zeros((128 - 2 * ep, rows), F32)
    theirs = jnp.concatenate([meta_in[...], blank], axis=0).T
    slot_theirs = theirs.astype(jnp.int32)
    for d in range(far, ep):
        if d > far:
            send_back(d, d - far).wait_recv()
        mix(
            d, res if d == far else back, slot_theirs, theirs[:, ep + d:ep + d + 1],
            d == far, joined if d == ep - 1 else None,
        )
    home = across(1, joined, joined_in)
    home.start()

    for d in range(far):
        if d > 0:
            send_back(d, d).wait_recv()
        mix(d, res if d == 0 else back, key, share[:, d:d + 1], d == 0, None)
    home.wait_recv()

    @pl.loop(0, width // tile)
    def _(j):
        c = pl.ds(pl.multiple_of(j * tile, tile), tile)
        o_ref[:, c] = (acc[:, c] + joined_in[:, c].astype(F32)).astype(BF16)

    for d in range(1, ep):
        send_rows(d).wait_send()
        if d < far:
            send_back(d, d).wait_send()
        elif d > far:
            send_back(d, d - far).wait_send()
    told.wait_send()
    home.wait_send()
    for c in passed:
        c.wait_send()


def fused_device(tokens, norm_gain, expert_ids, route_weights, w_gate, w_up, w_down):
    rows, width = tokens.shape
    ep = lax.axis_size("ep")
    tps = lax.axis_size("tp")
    slots = 3 * rows * expert_ids.shape[1] // (2 * ep)
    half = w_gate.shape[2]
    vm = pl.BlockSpec(memory_space=pltpu.VMEM)
    anywhere = pl.BlockSpec(memory_space=pl.ANY)
    dma = pltpu.SemaphoreType.DMA
    return pl.pallas_call(
        functools.partial(kernel, ep, slots),
        out_shape=jax.ShapeDtypeStruct((rows, width), BF16),
        in_specs=[vm, vm, vm, vm, anywhere, anywhere, anywhere],
        out_specs=vm,
        scratch_shapes=[
            pltpu.VMEM((tps, width, half), BF16),
            pltpu.VMEM((tps, width, half), BF16),
            pltpu.VMEM((tps * half, width), BF16),
            pltpu.VMEM((rows, width), BF16),
            pltpu.VMEM((ep * slots, width), BF16),
            pltpu.VMEM((ep * slots, width), BF16),
            pltpu.VMEM((2 * slots, tps * half), BF16),
            pltpu.VMEM((ep * slots, width), BF16),
            pltpu.VMEM((ep * slots, width), BF16),
            pltpu.VMEM((rows, width), F32),
            pltpu.VMEM((2 * ep, rows), F32),
            pltpu.VMEM((2 * ep, rows), F32),
            pltpu.VMEM((rows, width), BF16),
            pltpu.VMEM((rows, width), BF16),
            dma((3,)), dma((3,)), dma((3,)),
            dma((ep,)), dma((ep,)), dma((ep,)), dma((ep,)), dma((2,)), dma((2,)),
        ],
        compiler_params=pltpu.CompilerParams(
            collective_id=0, has_side_effects=True, vmem_limit_bytes=56 * 1024 * 1024
        ),
    )(tokens, norm_gain.reshape(1, -1), expert_ids, route_weights, w_gate, w_up, w_down)


def per_device(tokens, norm_gain, expert_ids, route_weights, w_gate, w_up, w_down):
    rows, width = tokens.shape
    ep = lax.axis_size("ep")
    slots = 3 * rows * expert_ids.shape[1] // (2 * ep)
    fits = (
        w_gate.shape[0] == 1
        and lax.axis_size("tp") == 2
        and ep & (ep - 1) == 0
        and 8 <= ep <= 32
        and slots % 16 == 0
        and rows % 128 == 0
        and width % 512 == 0
        and w_gate.shape[2] % 256 == 0
    )
    body = fused_device if fits else plain_device
    return body(tokens, norm_gain, expert_ids, route_weights, w_gate, w_up, w_down)


def solution(mesh):
    in_specs = (
        P(("grp", "ep", "tp"), None),
        P(),
        P(("grp", "ep", "tp"), None),
        P(("grp", "ep", "tp"), None),
        P("ep", None, "tp"),
        P("ep", None, "tp"),
        P("ep", "tp", None),
    )
    out_specs = P(("grp", "ep", "tp"), None)
    return jax.shard_map(
        per_device, mesh=mesh, in_specs=in_specs, out_specs=out_specs, check_vma=False
    )
```
